32 devices in a mesh: rep: 2 (over x), fs: 4 (over z), tp: 4 (over y, core).
Axes of the slice: x: 2, y: 2, z: 4, core: 2. Of those that a mesh axis runs over, the one named last changes fastest.
Arguments:
- tokens: bfloat16 [4096, 2048], P(('rep', 'fs', 'tp')), may hold values from -6 to 6
- norm_gain: float32 [2048], replicated, may hold values from 0.1 to 1.9
- gate_weight: float32 [2048, 5632], P('fs', 'tp'), may hold values from -0.125 to 0.125
- gate_scale: float32 [5632], P('tp'), may hold values from 0.5 to 2
- up_weight: float32 [2048, 5632], P('fs', 'tp'), may hold values from -0.125 to 0.125
- up_scale: float32 [5632], P('tp'), may hold values from 0.5 to 2
- down_weight: float32 [5632, 2048], P('tp', 'fs'), may hold values from -0.078125 to 0.078125
- down_scale: float32 [2048], P('fs'), may hold values from 0.5 to 2
Outputs:
- mixed: bfloat16 [4096, 2048], P(('rep', 'fs', 'tp'))
The draws below stay inside these ranges and needn't reach their ends.
All inputs are finite; a program needn't handle non-finite values.
Results may differ from the reference program's by a relative error of at most 0.014.
Values may be sent and summed in bfloat16 or wider, within the bound.
A program may use at most 64 MiB of HBM per device.

```python
import math
import jax
import jax.numpy as jnp
from jax import lax

D = 2048
FF = 5632
TOKENS = 4096
N_TP = 4


def block_levels(rng, dims, shards, low, top_value):
    def one(position, parts):
        steps = jax.random.uniform(jax.random.fold_in(jax.random.fold_in(rng, 6), position), (parts,), jnp.float32, low / len(shards), top_value / len(shards))
        return jnp.repeat(jnp.exp(steps), dims[position] // parts).reshape((-1,) + (1,) * (len(dims) - position - 1))

    factor_of = one(*shards[0])
    for cut in shards[1:]:
        factor_of = factor_of * one(*cut)
    return factor_of


def bell_draw(rng, shape, spread, limit, split=(), held_as=jnp.bfloat16):
    array = spread * jax.random.normal(rng, shape, jnp.float32)
    if split:
        array = array * block_levels(rng, shape, split, -0.22, 0.18)
    return jnp.clip(array, -limit, limit).astype(held_as)


def setup_inputs(seed: int = 0) -> dict:
    key_of = jax.random.split(jax.random.key(seed), 9)
    tokens = bell_draw(key_of[0], (TOKENS, D), 1.0, 6.0, ((0, 32),))
    norm_gain = jnp.clip(1.0 + 0.18 * jax.random.normal(key_of[1], (D,), jnp.float32), 0.1, 1.9)
    gate_weight = bell_draw(key_of[2], (D, FF), D ** -0.5, 0.125, ((0, 4), (1, 4)), jnp.float32)
    gate_scale = jnp.clip(jnp.exp(math.log(2.0) - 1.3862944 * jax.random.uniform(key_of[3], (FF,), jnp.float32) ** block_levels(key_of[3], (FF,), ((0, 4),), -0.2, 0.2)), 0.5, 2.0)
    up_weight = bell_draw(key_of[4], (D, FF), D ** -0.5, 0.125, ((0, 4), (1, 4)), jnp.float32)
    up_scale = jnp.clip(jnp.exp(math.log(2.0) - 1.3862944 * jax.random.uniform(key_of[5], (FF,), jnp.float32) ** block_levels(key_of[5], (FF,), ((0, 4),), -0.2, 0.2)), 0.5, 2.0)
    down_weight = bell_draw(key_of[6], (FF, D), FF ** -0.5, 0.078125, ((0, 4), (1, 4)), jnp.float32)
    down_scale = jnp.clip(jnp.exp(math.log(2.0) - 1.3862944 * jax.random.uniform(key_of[7], (D,), jnp.float32) ** block_levels(key_of[7], (D,), ((0, 4),), -0.2, 0.2)), 0.5, 2.0)
    return dict(tokens=tokens, norm_gain=norm_gain, gate_weight=gate_weight, gate_scale=gate_scale, up_weight=up_weight, up_scale=up_scale, down_weight=down_weight, down_scale=down_scale)


def reference(tokens, norm_gain, gate_weight, gate_scale, up_weight, up_scale, down_weight, down_scale):
    flat = tokens.astype(jnp.float32)
    mean_square = lax.optimization_barrier(jnp.mean(flat * flat, axis=-1, keepdims=True))
    inverse = jax.lax.rsqrt(mean_square + 1e-06)
    normed = (flat * inverse * norm_gain).astype(jnp.bfloat16)
    gate_low = gate_weight.astype(jnp.bfloat16)
    up_low = up_weight.astype(jnp.bfloat16)
    down_low = down_weight.astype(jnp.bfloat16)
    gate = jnp.dot(normed, gate_low, preferred_element_type=jnp.float32) * gate_scale
    up = jnp.dot(normed, up_low, preferred_element_type=jnp.float32) * up_scale
    hidden = (jax.nn.silu(gate) * up).astype(jnp.bfloat16)
    width = FF // N_TP
    total = jnp.zeros((tokens.shape[0], D), jnp.float32)
    for block in range(N_TP):
        part = jnp.dot(hidden[:, block * width:(block + 1) * width], down_low[block * width:(block + 1) * width, :], preferred_element_type=jnp.float32)
        total = total + part.astype(jnp.bfloat16).astype(jnp.float32)
    return (total * down_scale).astype(jnp.bfloat16)
```

```python
import jax
import jax.numpy as jnp
from jax import lax
from jax.sharding import PartitionSpec as P


def shards(
    tokens, norm_gain, gate_weight, gate_scale, up_weight, up_scale, down_weight, down_scale
):
    n_rep = lax.axis_size("rep")
    rep = lax.axis_index("rep")
    width = gate_weight.shape[1] // n_rep
    start = rep * width

    def part(array, axis):
        return lax.dynamic_slice_in_dim(array, start, width, axis)

    flat = tokens.astype(jnp.float32)
    mean_square = jnp.mean(flat * flat, axis=-1, keepdims=True)
    inverse = lax.rsqrt(mean_square + 1e-06)
    normed = (flat * inverse * norm_gain).astype(jnp.bfloat16)
    group = lax.all_gather(normed, ("rep", "tp"), axis=0, tiled=True)
    gate_low = part(gate_weight, 1).astype(jnp.bfloat16)
    up_low = part(up_weight, 1).astype(jnp.bfloat16)
    down_low = part(down_weight, 0).astype(jnp.bfloat16)
    gate = jnp.dot(
        group,
        lax.all_gather(gate_low, "fs", axis=0, tiled=True),
        preferred_element_type=jnp.float32,
    )
    up = jnp.dot(
        group, lax.all_gather(up_low, "fs", axis=0, tiled=True), preferred_element_type=jnp.float32
    )
    down_full = lax.all_gather(down_low, "fs", axis=1, tiled=True)
    gate = gate * part(gate_scale, 0)
    up = up * part(up_scale, 0)
    hidden = (jax.nn.silu(gate) * up).astype(jnp.bfloat16)
    scales = lax.all_gather(down_scale, "fs", axis=0, tiled=True)
    total = lax.psum_scatter(
        jnp.dot(hidden, down_full, preferred_element_type=jnp.float32).astype(jnp.bfloat16),
        ("rep", "tp"),
        scatter_dimension=0,
        tiled=True,
    ).astype(jnp.float32)
    return (total * scales).astype(jnp.bfloat16)


def solution(mesh):
    in_specs = (
        P(("rep", "fs", "tp"), None),
        P(),
        P("fs", "tp"),
        P("tp"),
        P("fs", "tp"),
        P("tp"),
        P("tp", "fs"),
        P("fs"),
    )
    out_specs = P(("rep", "fs", "tp"), None)
    return jax.shard_map(shards, mesh=mesh, in_specs=in_specs, out_specs=out_specs, check_vma=False)
```

```python
import functools

import jax
import jax.numpy as jnp
from jax import lax
from jax.experimental import pallas as pl
from jax.experimental.pallas import tpu as pltpu
from jax.sharding import PartitionSpec as P

MESH = pl.DeviceIdType.MESH


def layer(
    n_rep,
    n_fs,
    n_tp,
    tok_ref,
    gu_ref,
    dn_ref,
    gs_ref,
    us_ref,
    ds_ref,
    out_ref,
    tok_all,
    gu_all,
    dn_all,
    sc_all,
    acc,
    hidden,
    parts,
    landed,
    tok_send,
    tok_recv,
    gu_send,
    gu_recv,
    dn_send,
    dn_recv,
    sc_send,
    sc_recv,
    part_send,
    part_recv,
):
    rep, fs, tp = lax.axis_index("rep"), lax.axis_index("fs"), lax.axis_index("tp")
    peers = n_rep * n_tp
    me = rep * n_tp + tp
    rows = tok_ref.shape[0]
    depth = gu_ref.shape[0]
    half = gu_ref.shape[1] // 2
    cols = dn_ref.shape[1]
    last = n_fs - 1

    def plane(peer):
        return (peer // n_tp, fs, peer % n_tp)

    barrier = pltpu.get_barrier_semaphore()
    for hop in (1, n_fs - 1):
        pl.semaphore_signal(
            barrier, inc=1, device_id=(rep, (fs + hop) % n_fs, tp), device_id_type=MESH
        )
    for hop in range(1, peers):
        pl.semaphore_signal(
            barrier, inc=1, device_id=plane((me + hop) % peers), device_id_type=MESH
        )
    pl.semaphore_wait(barrier, peers + 1)

    def side(own, store, send, recv, source, way, first):
        return pltpu.make_async_remote_copy(
            src_ref=own if first else store.at[source],
            dst_ref=store.at[source],
            send_sem=send.at[way, source],
            recv_sem=recv.at[source],
            device_id=(rep, (fs + (1, n_fs - 1)[way]) % n_fs, tp),
            device_id_type=MESH,
        )

    gu_side = functools.partial(side, gu_ref, gu_all, gu_send, gu_recv)
    dn_side = functools.partial(side, dn_ref, dn_all, dn_send, dn_recv)
    sc_side = functools.partial(side, ds_ref, sc_all, sc_send, sc_recv)

    def own_copies(make, way, act):
        @pl.when(fs < last if way == 0 else fs > 0)
        def _():
            act(make(fs, way, True))

    def start(copy):
        copy.start()

    def tok_copy(hop):
        peer = (me + hop) % peers
        return pltpu.make_async_remote_copy(
            src_ref=tok_ref,
            dst_ref=tok_all.at[pl.ds(pl.multiple_of(me * rows, rows), rows), :],
            send_sem=tok_send.at[peer],
            recv_sem=tok_recv.at[me],
            device_id=plane(peer),
            device_id_type=MESH,
        )

    def tok_arrival(peer):
        return pltpu.make_async_remote_copy(
            src_ref=tok_ref,
            dst_ref=tok_all.at[pl.ds(pl.multiple_of(peer * rows, rows), rows), :],
            send_sem=tok_send.at[peer],
            recv_sem=tok_recv.at[peer],
            device_id=plane(peer),
            device_id_type=MESH,
        )

    for way in (0, 1):
        own_copies(gu_side, way, start)
    for hop in range(1, peers):
        tok_copy(hop).start()
    for way in (0, 1):
        own_copies(sc_side, way, start)

    @pl.when(fs == 0)
    def _():
        own_copies(dn_side, 0, start)

    @pl.when(fs == last)
    def _():
        own_copies(dn_side, 1, start)

    tok_all[pl.ds(pl.multiple_of(me * rows, rows), rows), :] = tok_ref[...]

    def arrive(make, source, way):
        make(source, way, False).wait_recv()

        @pl.when(fs < last if way == 0 else fs > 0)
        def _():
            make(source, way, False).start()

    tile = 2 * rows
    tiles = peers // 2

    def gather_step(step):
        from_left, from_right = fs - step, fs + step

        @pl.when(from_left >= 0)
        def _():
            arrive(gu_side, from_left, 0)

            @pl.when(from_left == 0)
            def _():
                own_copies(dn_side, 0, start)

        @pl.when(from_right <= last)
        def _():
            arrive(gu_side, from_right, 1)

            @pl.when(from_right == last)
            def _():
                own_copies(dn_side, 1, start)

    def accumulate(source, weights, fresh):
        def body(j, carry):
            r = pl.ds(pl.multiple_of(j * tile, tile), tile)
            k = pl.ds(pl.multiple_of(source * depth, depth), depth)
            got = jnp.dot(tok_all[r, k], weights[...], preferred_element_type=jnp.float32)
            acc[r, :] = got if fresh else acc[r, :] + got
            return carry

        lax.fori_loop(0, tiles, body, 0)

    gather_step(1)
    for hop in range(1, peers):
        tok_arrival((me + hop) % peers).wait_recv()
    accumulate(fs, gu_ref, True)

    def gu_step(step, carry):
        @pl.when(step > 1)
        def _():
            gather_step(step)

        @pl.when(fs - step >= 0)
        def _():
            accumulate(fs - step, gu_all.at[fs - step], False)

        @pl.when(fs + step <= last)
        def _():
            accumulate(fs + step, gu_all.at[fs + step], False)

        return carry

    lax.fori_loop(1, n_fs, gu_step, 0)

    def activate(j, carry):
        r = pl.ds(pl.multiple_of(j * rows, rows), rows)
        both = acc[r, :]
        gate = both[:, :half] * gs_ref[...]
        up = both[:, half:] * us_ref[...]
        hidden[r, :] = (gate / (1.0 + jnp.exp(-gate)) * up).astype(jnp.bfloat16)
        return carry

    lax.fori_loop(0, peers, activate, 0)

    def part_copy(source, peer):
        return pltpu.make_async_remote_copy(
            src_ref=parts.at[source, pl.ds(pl.multiple_of(peer * rows, rows), rows), :],
            dst_ref=landed.at[source, me],
            send_sem=part_send.at[source, peer],
            recv_sem=part_recv.at[source, me],
            device_id=plane(peer),
            device_id_type=MESH,
        )

    def part_arrival(source, peer):
        return pltpu.make_async_remote_copy(
            src_ref=parts.at[source, pl.ds(pl.multiple_of(peer * rows, rows), rows), :],
            dst_ref=landed.at[source, peer],
            send_sem=part_send.at[source, peer],
            recv_sem=part_recv.at[source, peer],
            device_id=plane(peer),
            device_id_type=MESH,
        )

    def project(source, weights):
        def body(j, carry):
            r = pl.ds(pl.multiple_of(j * tile, tile), tile)
            parts[source, r, :] = jnp.dot(
                hidden[r, :], weights[...], preferred_element_type=jnp.float32
            ).astype(jnp.bfloat16)
            for k in (0, 1):
                peer = j * 2 + k

                @pl.when(peer != me)
                def _():
                    part_copy(source, peer).start()

            return carry

        lax.fori_loop(0, tiles, body, 0)

    def finish(source, scale):
        total = parts[source, pl.ds(pl.multiple_of(me * rows, rows), rows), :].astype(jnp.float32)

        def add(hop, total):
            peer = (me + hop) % peers
            part_arrival(source, peer).wait_recv()
            return total + landed[source, peer].astype(jnp.float32)

        for hop in range(1, peers):
            total = add(hop, total)
        out_ref[:, pl.ds(pl.multiple_of(source * cols, cols), cols)] = (total * scale).astype(
            jnp.bfloat16
        )

    project(fs, dn_ref)

    def dn_step(step, carry):
        from_left, from_right = fs - step, fs + step

        @pl.when(from_left >= 0)
        def _():
            arrive(sc_side, from_left, 0)
            arrive(dn_side, from_left, 0)

        @pl.when(from_right <= last)
        def _():
            arrive(sc_side, from_right, 1)
            arrive(dn_side, from_right, 1)

        @pl.when(from_left >= 0)
        def _():
            project(from_left, dn_all.at[from_left])

        @pl.when(from_right <= last)
        def _():
            project(from_right, dn_all.at[from_right])

        return carry

    lax.fori_loop(1, n_fs, dn_step, 0)

    finish(fs, ds_ref[0:1, :])

    def end_step(step, carry):
        for source in (fs - step, fs + step):

            @pl.when((source >= 0) & (source <= last))
            def _():
                finish(source, sc_all[source, 0:1, :])

        return carry

    lax.fori_loop(1, n_fs, end_step, 0)

    def sent_step(source, carry):
        for make in (gu_side, dn_side, sc_side):

            @pl.when((source <= fs) & (fs < last))
            def _():
                make(source, 0, False).wait_send()

            @pl.when((source >= fs) & (fs > 0))
            def _():
                make(source, 1, False).wait_send()

        for hop in range(1, peers):
            part_copy(source, (me + hop) % peers).wait_send()
        return carry

    lax.fori_loop(0, n_fs, sent_step, 0)
    for hop in range(1, peers):
        tok_copy(hop).wait_send()


def shards(
    sizes,
    tokens,
    norm_gain,
    gate_weight,
    gate_scale,
    up_weight,
    up_scale,
    down_weight,
    down_scale,
):
    n_rep, n_fs, n_tp = sizes
    peers = n_rep * n_tp
    width = gate_weight.shape[1] // n_rep
    begin = lax.axis_index("rep") * width

    def part(array, axis):
        return lax.dynamic_slice_in_dim(array, begin, width, axis)

    flat = tokens.astype(jnp.float32)
    mean_square = jnp.mean(flat * flat, axis=-1, keepdims=True)
    inverse = lax.rsqrt(mean_square + 1e-06)
    normed = (flat * inverse * norm_gain).astype(jnp.bfloat16)
    gu = jnp.concatenate(
        [part(gate_weight, 1).astype(jnp.bfloat16), part(up_weight, 1).astype(jnp.bfloat16)], axis=1
    )
    dn = part(down_weight, 0).astype(jnp.bfloat16)
    scale = jnp.broadcast_to(down_scale[None, :], (8, down_scale.shape[0]))
    rows, features = tokens.shape
    depth = gu.shape[0]
    cols = dn.shape[1]
    dma = pltpu.SemaphoreType.DMA
    vmem = pl.BlockSpec(memory_space=pltpu.VMEM)
    return pl.pallas_call(
        functools.partial(layer, n_rep, n_fs, n_tp),
        out_shape=jax.ShapeDtypeStruct((rows, features), jnp.bfloat16),
        in_specs=[vmem] * 6,
        out_specs=vmem,
        scratch_shapes=[
            pltpu.VMEM((peers * rows, features), jnp.bfloat16),
            pltpu.VMEM((n_fs, depth, 2 * width), jnp.bfloat16),
            pltpu.VMEM((n_fs, width, cols), jnp.bfloat16),
            pltpu.VMEM((n_fs, 8, cols), jnp.float32),
            pltpu.VMEM((peers * rows, 2 * width), jnp.float32),
            pltpu.VMEM((peers * rows, width), jnp.bfloat16),
            pltpu.VMEM((n_fs, peers * rows, cols), jnp.bfloat16),
            pltpu.VMEM((n_fs, peers, rows, cols), jnp.bfloat16),
            dma((peers,)),
            dma((peers,)),
            dma((2, n_fs)),
            dma((n_fs,)),
            dma((2, n_fs)),
            dma((n_fs,)),
            dma((2, n_fs)),
            dma((n_fs,)),
            dma((n_fs, peers)),
            dma((n_fs, peers)),
        ],
        compiler_params=pltpu.CompilerParams(
            collective_id=0, has_side_effects=True, vmem_limit_bytes=60 * 1024 * 1024
        ),
    )(normed, gu, dn, part(gate_scale, 0)[None, :], part(up_scale, 0)[None, :], scale)


def solution(mesh):
    in_specs = (
        P(("rep", "fs", "tp"), None),
        P(),
        P("fs", "tp"),
        P("tp"),
        P("fs", "tp"),
        P("tp"),
        P("tp", "fs"),
        P("fs"),
    )
    out_specs = P(("rep", "fs", "tp"), None)
    sizes = tuple(mesh.shape[axis] for axis in ("rep", "fs", "tp"))
    return jax.shard_map(
        functools.partial(shards, sizes),
        mesh=mesh,
        in_specs=in_specs,
        out_specs=out_specs,
        check_vma=False,
    )
```

```python
import functools

import jax
import jax.numpy as jnp
from jax import lax
from jax.experimental import pallas as pl
from jax.experimental.pallas import tpu as pltpu
from jax.sharding import PartitionSpec as P

MESH = pl.DeviceIdType.MESH


def layer(
    n_rep,
    n_fs,
    n_tp,
    tok_ref,
    gu_ref,
    dn_ref,
    hs_ref,
    ds_ref,
    out_ref,
    tok_all,
    gu_all,
    dn_all,
    sc_all,
    hs_all,
    acc,
    hidden,
    parts,
    landed,
    back,
    tok_send,
    tok_recv,
    gu_send,
    gu_recv,
    dn_send,
    dn_recv,
    sc_send,
    sc_recv,
    gu_sib_send,
    gu_sib_recv,
    dn_sib_send,
    dn_sib_recv,
    hs_sem,
    part_send,
    part_recv,
    back_send,
    back_recv,
    tok_z_send,
):
    rep, fs, tp = lax.axis_index("rep"), lax.axis_index("fs"), lax.axis_index("tp")
    n_row = n_tp // 2
    core = tp % 2
    chips = n_rep * n_row
    me = rep * n_row + tp // 2
    rows = tok_ref.shape[0]
    depth = gu_ref.shape[0]
    half = gu_ref.shape[1] // 2
    cols = dn_ref.shape[1]
    low, high, last = 1, n_fs - 2, n_fs - 1
    pair = fs // 2
    parity = fs % 2
    upper = jnp.where(pair < n_fs // 4, 0, 1)
    works = parity + upper == 1
    inside = (fs >= low) & (fs <= high)
    partner = (rep, fs + 1 - 2 * parity, tp)
    sibling = (rep, fs, tp + 1 - 2 * core)

    def chip(index):
        return (index // n_row, fs, (index % n_row) * 2 + core)

    barrier = pltpu.get_barrier_semaphore()
    for hop in (1, n_fs - 1):
        pl.semaphore_signal(
            barrier, inc=1, device_id=(rep, (fs + hop) % n_fs, tp), device_id_type=MESH
        )
    pl.semaphore_signal(barrier, inc=1, device_id=sibling, device_id_type=MESH)
    for hop in range(1, chips):
        pl.semaphore_signal(
            barrier, inc=1, device_id=chip((me + hop) % chips), device_id_type=MESH
        )
    pl.semaphore_wait(barrier, chips + 2)

    def remote(src, dst, send, recv, device):
        return pltpu.make_async_remote_copy(
            src_ref=src,
            dst_ref=dst,
            send_sem=send,
            recv_sem=recv,
            device_id=device,
            device_id_type=MESH,
        )

    def block(index):
        return pl.ds(pl.multiple_of(index * rows, rows), rows)

    def side(own, store, send, recv, source, way, first):
        return remote(
            own if first else store.at[source],
            store.at[source],
            send.at[way, source],
            recv.at[source],
            (rep, (fs + (1, n_fs - 1)[way]) % n_fs, tp),
        )

    gu_side = functools.partial(side, gu_ref, gu_all.at[0], gu_send, gu_recv)
    dn_side = functools.partial(side, dn_ref, dn_all.at[0], dn_send, dn_recv)
    sc_side = functools.partial(side, ds_ref, sc_all, sc_send, sc_recv)

    def sib(own, store, send, recv, source, first):
        return remote(
            own if first else store.at[0, source],
            store.at[1, source],
            send.at[source],
            recv.at[source],
            sibling,
        )

    gu_sib = functools.partial(sib, gu_ref, gu_all, gu_sib_send, gu_sib_recv)
    dn_sib = functools.partial(sib, dn_ref, dn_all, dn_sib_send, dn_sib_recv)
    hs_copy = remote(hs_ref, hs_all, hs_sem.at[0], hs_sem.at[1], sibling)

    def goes(way):
        return fs < high if way == 0 else fs > low

    def own_copies(make, way):
        @pl.when(goes(way))
        def _():
            make(fs, way, True).start()

    def tok_copy(plane, hop):
        to = (me + hop) % chips
        home = tok_all.at[block(plane * chips + me), :]
        return remote(
            tok_ref if plane == 0 else home,
            home,
            tok_send.at[plane, to],
            tok_recv.at[plane, me],
            chip(to),
        )

    def tok_arrival(plane, index):
        home = tok_all.at[block(plane * chips + index), :]
        return remote(
            home, home, tok_send.at[plane, index], tok_recv.at[plane, index], chip(index)
        )

    tok_z = remote(
        tok_ref, tok_all.at[block(chips + me), :], tok_z_send, tok_recv.at[1, me], partner
    )

    @pl.when(jnp.logical_not(works))
    def _():
        tok_z.start()

    for way in (0, 1):
        own_copies(gu_side, way)

    @pl.when(works)
    def _():
        for hop in range(1, chips):
            tok_copy(0, hop).start()
        hs_copy.start()
        gu_sib(fs, True).start()
        dn_sib(fs, True).start()

    for way in (0, 1):
        own_copies(sc_side, way)

    @pl.when(fs == 0)
    def _():
        own_copies(dn_side, 0)

    @pl.when(fs == last)
    def _():
        own_copies(dn_side, 1)

    @pl.when(works)
    def _():
        tok_all[block(me), :] = tok_ref[...]
        tok_z.wait_recv()
        for hop in range(1, chips):
            tok_copy(1, hop).start()

    def arrive(make, source, way, to_sibling):
        make(source, way, False).wait_recv()

        @pl.when(goes(way))
        def _():
            make(source, way, False).start()

        if to_sibling is not None:

            @pl.when(works)
            def _():
                to_sibling(source, False).start()

    tile = 2 * rows
    tiles = chips

    def left_ok(step):
        return inside & (fs - step >= 0)

    def right_ok(step):
        return inside & (fs + step <= last)

    def gather_step(step):
        from_left, from_right = fs - step, fs + step

        @pl.when(left_ok(step))
        def _():
            arrive(gu_side, from_left, 0, gu_sib)

            @pl.when(from_left == 0)
            def _():
                own_copies(dn_side, 0)

        @pl.when(right_ok(step))
        def _():
            arrive(gu_side, from_right, 1, gu_sib)

            @pl.when(from_right == last)
            def _():
                own_copies(dn_side, 1)

    def accumulate(source, weights, fresh):
        gu_sib(source, False).wait_recv()

        def body(j, carry):
            r = pl.ds(pl.multiple_of(j * tile, tile), tile)
            k = pl.ds(pl.multiple_of(source * depth, depth), depth)
            for c, block_of in ((0, weights), (1, gu_all.at[1, source])):
                got = jnp.dot(tok_all[r, k], block_of[...], preferred_element_type=jnp.float32)
                acc[c, r, :] = got if fresh else acc[c, r, :] + got
            return carry

        lax.fori_loop(0, tiles, body, 0)

    gather_step(1)

    @pl.when(works)
    def _():
        for hop in range(1, chips):
            for plane in (0, 1):
                tok_arrival(plane, (me + hop) % chips).wait_recv()
        accumulate(fs, gu_ref, True)

    def gu_step(step, carry):
        @pl.when(step > 1)
        def _():
            gather_step(step)

        @pl.when(works & left_ok(step))
        def _():
            accumulate(fs - step, gu_all.at[0, fs - step], False)

        @pl.when(works & right_ok(step))
        def _():
            accumulate(fs + step, gu_all.at[0, fs + step], False)

        return carry

    lax.fori_loop(1, n_fs, gu_step, 0)

    @pl.when(works)
    def _():
        hs_copy.wait_recv()

        def activate(j, carry):
            r = block(j)
            for c, scale in ((0, hs_ref), (1, hs_all)):
                both = acc[c, r, :] * scale[0:1, :]
                gate, up = both[:, :half], both[:, half:]
                hidden[c, r, :] = (gate / (1.0 + jnp.exp(-gate)) * up).astype(jnp.bfloat16)
            return carry

        lax.fori_loop(0, 2 * chips, activate, 0)

    def part_copy(source, plane, to):
        return remote(
            parts.at[source, block(plane * chips + to), :],
            landed.at[source, plane, me],
            part_send.at[source, plane, to],
            part_recv.at[source, plane, me],
            chip(to),
        )

    def part_arrival(source, plane, index):
        return remote(
            parts.at[source, block(plane * chips + index), :],
            landed.at[source, plane, index],
            part_send.at[source, plane, index],
            part_recv.at[source, plane, index],
            chip(index),
        )

    def project(source, weights):
        dn_sib(source, False).wait_recv()

        def body(i, carry):
            j = tiles - 1 - i
            r = pl.ds(pl.multiple_of(j * tile, tile), tile)
            parts[source, r, :] = (
                jnp.dot(hidden[0, r, :], weights[...], preferred_element_type=jnp.float32)
                + jnp.dot(
                    hidden[1, r, :], dn_all[1, source], preferred_element_type=jnp.float32
                )
            ).astype(jnp.bfloat16)
            for k in (0, 1):
                index = j * 2 + k

                @pl.when(index % chips != me)
                def _():
                    part_copy(source, index // chips, index % chips).start()

            return carry

        lax.fori_loop(0, tiles, body, 0)

    def back_copy(source):
        return remote(
            back.at[source], back.at[source], back_send.at[source], back_recv.at[source], partner
        )

    def finish(source, scale):
        for plane in (1, 0):
            total = parts[source, block(plane * chips + me), :].astype(jnp.float32)
            for hop in range(1, chips):
                index = (me + hop) % chips
                part_arrival(source, plane, index).wait_recv()
                total = total + landed[source, plane, index].astype(jnp.float32)
            mixed = (total * scale).astype(jnp.bfloat16)
            if plane == 1:
                back[source] = mixed
                back_copy(source).start()
            else:
                out_ref[:, pl.ds(pl.multiple_of(source * cols, cols), cols)] = mixed

    @pl.when(works)
    def _():
        project(fs, dn_ref)

    def dn_step(step, carry):
        from_left, from_right = fs - step, fs + step

        @pl.when(left_ok(step))
        def _():
            arrive(sc_side, from_left, 0, None)
            arrive(dn_side, from_left, 0, dn_sib)

        @pl.when(right_ok(step))
        def _():
            arrive(sc_side, from_right, 1, None)
            arrive(dn_side, from_right, 1, dn_sib)

        @pl.when(works & left_ok(step))
        def _():
            project(from_left, dn_all.at[0, from_left])

        @pl.when(works & right_ok(step))
        def _():
            project(from_right, dn_all.at[0, from_right])

        return carry

    lax.fori_loop(1, n_fs, dn_step, 0)

    @pl.when(works)
    def _():
        finish(fs, ds_ref[0:1, :])

    def end_step(step, carry):
        for source, ok in ((fs - step, left_ok(step)), (fs + step, right_ok(step))):

            @pl.when(works & ok)
            def _():
                finish(source, sc_all[source, 0:1, :])

        return carry

    lax.fori_loop(1, n_fs, end_step, 0)

    @pl.when(jnp.logical_not(works))
    def _():
        tok_z.wait_send()

        def take(source, carry):
            back_copy(source).wait_recv()
            out_ref[:, pl.ds(pl.multiple_of(source * cols, cols), cols)] = back[source]
            return carry

        lax.fori_loop(0, n_fs, take, 0)

    def sent_step(source, carry):
        for make in (gu_side, dn_side, sc_side):

            @pl.when((source <= fs) & goes(0))
            def _():
                make(source, 0, False).wait_send()

            @pl.when((source >= fs) & goes(1))
            def _():
                make(source, 1, False).wait_send()

        @pl.when(works)
        def _():
            gu_sib(source, False).wait_send()
            dn_sib(source, False).wait_send()
            back_copy(source).wait_send()
            for hop in range(1, chips):
                for plane in (0, 1):
                    part_copy(source, plane, (me + hop) % chips).wait_send()

        return carry

    lax.fori_loop(0, n_fs, sent_step, 0)

    @pl.when(works)
    def _():
        hs_copy.wait_send()
        for hop in range(1, chips):
            for plane in (0, 1):
                tok_copy(plane, hop).wait_send()


def shards(
    sizes,
    tokens,
    norm_gain,
    gate_weight,
    gate_scale,
    up_weight,
    up_scale,
    down_weight,
    down_scale,
):
    n_rep, n_fs, n_tp = sizes
    chips = n_rep * n_tp // 2
    width = gate_weight.shape[1] // n_rep
    begin = lax.axis_index("rep") * width

    def part(array, axis):
        return lax.dynamic_slice_in_dim(array, begin, width, axis)

    flat = tokens.astype(jnp.float32)
    mean_square = jnp.mean(flat * flat, axis=-1, keepdims=True)
    inverse = lax.rsqrt(mean_square + 1e-06)
    normed = (flat * inverse * norm_gain).astype(jnp.bfloat16)
    gu = jnp.concatenate(
        [part(gate_weight, 1).astype(jnp.bfloat16), part(up_weight, 1).astype(jnp.bfloat16)], axis=1
    )
    dn = part(down_weight, 0).astype(jnp.bfloat16)
    scale = jnp.broadcast_to(down_scale[None, :], (8, down_scale.shape[0]))
    hidden_scale = jnp.concatenate([part(gate_scale, 0), part(up_scale, 0)])
    hidden_scale = jnp.broadcast_to(hidden_scale[None, :], (8, 2 * width))
    rows, features = tokens.shape
    depth = gu.shape[0]
    cols = dn.shape[1]
    dma = pltpu.SemaphoreType.DMA
    vmem = pl.BlockSpec(memory_space=pltpu.VMEM)
    return pl.pallas_call(
        functools.partial(layer, n_rep, n_fs, n_tp),
        out_shape=jax.ShapeDtypeStruct((rows, features), jnp.bfloat16),
        in_specs=[vmem] * 5,
        out_specs=vmem,
        scratch_shapes=[
            pltpu.VMEM((2 * chips * rows, features), jnp.bfloat16),
            pltpu.VMEM((2, n_fs, depth, 2 * width), jnp.bfloat16),
            pltpu.VMEM((2, n_fs, width, cols), jnp.bfloat16),
            pltpu.VMEM((n_fs, 8, cols), jnp.float32),
            pltpu.VMEM((8, 2 * width), jnp.float32),
            pltpu.VMEM((2, 2 * chips * rows, 2 * width), jnp.float32),
            pltpu.VMEM((2, 2 * chips * rows, width), jnp.bfloat16),
            pltpu.VMEM((n_fs, 2 * chips * rows, cols), jnp.bfloat16),
            pltpu.VMEM((n_fs, 2, chips, rows, cols), jnp.bfloat16),
            pltpu.VMEM((n_fs, rows, cols), jnp.bfloat16),
            dma((2, chips)),
            dma((2, chips)),
            dma((2, n_fs)),
            dma((n_fs,)),
            dma((2, n_fs)),
            dma((n_fs,)),
            dma((2, n_fs)),
            dma((n_fs,)),
            dma((n_fs,)),
            dma((n_fs,)),
            dma((n_fs,)),
            dma((n_fs,)),
            dma((2,)),
            dma((n_fs, 2, chips)),
            dma((n_fs, 2, chips)),
            dma((n_fs,)),
            dma((n_fs,)),
            dma,
        ],
        compiler_params=pltpu.CompilerParams(
            collective_id=0, has_side_effects=True, vmem_limit_bytes=60 * 1024 * 1024
        ),
    )(normed, gu, dn, hidden_scale, scale)


def solution(mesh):
    in_specs = (
        P(("rep", "fs", "tp"), None),
        P(),
        P("fs", "tp"),
        P("tp"),
        P("fs", "tp"),
        P("tp"),
        P("tp", "fs"),
        P("fs"),
    )
    out_specs = P(("rep", "fs", "tp"), None)
    sizes = tuple(mesh.shape[axis] for axis in ("rep", "fs", "tp"))
    return jax.shard_map(
        functools.partial(shards, sizes),
        mesh=mesh,
        in_specs=in_specs,
        out_specs=out_specs,
        check_vma=False,
    )
```

```python
import functools

import jax
import jax.numpy as jnp
from jax import lax
from jax.experimental import pallas as pl
from jax.experimental.pallas import tpu as pltpu
from jax.sharding import PartitionSpec as P

MESH = pl.DeviceIdType.MESH


def layer(
    n_rep,
    n_fs,
    n_tp,
    tok_ref,
    gu_ref,
    dn_ref,
    hs_ref,
    ds_ref,
    out_ref,
    tok_all,
    gu_all,
    dn_all,
    sc_all,
    hs_all,
    acc,
    hidden,
    parts,
    landed,
    back,
    tok_send,
    tok_recv,
    gu_send,
    gu_recv,
    dn_send,
    dn_recv,
    sc_send,
    sc_recv,
    gu_sib_send,
    gu_sib_recv,
    dn_sib_send,
    dn_sib_recv,
    hs_sem,
    part_send,
    part_recv,
    back_send,
    back_recv,
    tok_z_send,
):
    rep, fs, tp = lax.axis_index("rep"), lax.axis_index("fs"), lax.axis_index("tp")
    n_row = n_tp // 2
    core = tp % 2
    chips = n_rep * n_row
    me = rep * n_row + tp // 2
    rows = tok_ref.shape[0]
    pieces = gu_ref.shape[0]
    depth = gu_ref.shape[1]
    half = gu_ref.shape[2] // 2
    cols = dn_ref.shape[1]
    low, high, last = 1, n_fs - 2, n_fs - 1
    pair = fs // 2
    parity = fs % 2
    upper = jnp.where(pair < n_fs // 4, 0, 1)
    works = parity + upper == 1
    inside = (fs >= low) & (fs <= high)
    partner = (rep, fs + 1 - 2 * parity, tp)
    sibling = (rep, fs, tp + 1 - 2 * core)

    def chip(index):
        return (index // n_row, fs, (index % n_row) * 2 + core)

    barrier = pltpu.get_barrier_semaphore()
    for hop in (1, n_fs - 1):
        pl.semaphore_signal(
            barrier, inc=1, device_id=(rep, (fs + hop) % n_fs, tp), device_id_type=MESH
        )
    pl.semaphore_signal(barrier, inc=1, device_id=sibling, device_id_type=MESH)
    for hop in range(1, chips):
        pl.semaphore_signal(
            barrier, inc=1, device_id=chip((me + hop) % chips), device_id_type=MESH
        )
    pl.semaphore_wait(barrier, chips + 2)

    def remote(src, dst, send, recv, device):
        return pltpu.make_async_remote_copy(
            src_ref=src,
            dst_ref=dst,
            send_sem=send,
            recv_sem=recv,
            device_id=device,
            device_id_type=MESH,
        )

    def block(index):
        return pl.ds(pl.multiple_of(index * rows, rows), rows)

    def side(own, store, send, recv, source, way, first):
        return remote(
            own if first else store.at[source],
            store.at[source],
            send.at[way, source],
            recv.at[source],
            (rep, (fs + (1, n_fs - 1)[way]) % n_fs, tp),
        )

    def gu_side(piece, source, way, first):
        unit = source * pieces + piece
        return remote(
            gu_ref.at[piece] if first else gu_all.at[0, unit],
            gu_all.at[0, unit],
            gu_send.at[way, unit],
            gu_recv.at[unit],
            (rep, (fs + (1, n_fs - 1)[way]) % n_fs, tp),
        )

    dn_side = functools.partial(side, dn_ref, dn_all.at[0], dn_send, dn_recv)
    sc_side = functools.partial(side, ds_ref, sc_all, sc_send, sc_recv)

    def sib(own, store, send, recv, source, first):
        return remote(
            own if first else store.at[0, source],
            store.at[1, source],
            send.at[source],
            recv.at[source],
            sibling,
        )

    def gu_sib(piece, source, first):
        unit = source * pieces + piece
        return sib(gu_ref.at[piece], gu_all, gu_sib_send, gu_sib_recv, unit, first)

    def gu_part(piece):
        return functools.partial(gu_side, piece), functools.partial(gu_sib, piece)

    dn_sib = functools.partial(sib, dn_ref, dn_all, dn_sib_send, dn_sib_recv)
    hs_copy = remote(hs_ref, hs_all, hs_sem.at[0], hs_sem.at[1], sibling)

    def goes(way):
        return fs < high if way == 0 else fs > low

    def own_copies(make, way):
        @pl.when(goes(way))
        def _():
            make(fs, way, True).start()

    def tok_copy(plane, hop):
        to = (me + hop) % chips
        home = tok_all.at[block(plane * chips + me), :]
        return remote(
            tok_ref if plane == 0 else home,
            home,
            tok_send.at[plane, to],
            tok_recv.at[plane, me],
            chip(to),
        )

    def tok_arrival(plane, index):
        home = tok_all.at[block(plane * chips + index), :]
        return remote(
            home, home, tok_send.at[plane, index], tok_recv.at[plane, index], chip(index)
        )

    tok_z = remote(
        tok_ref, tok_all.at[block(chips + me), :], tok_z_send, tok_recv.at[1, me], partner
    )

    for piece in range(pieces):
        for way in (0, 1):
            own_copies(gu_part(piece)[0], way)
        if piece == 0:

            @pl.when(jnp.logical_not(works))
            def _():
                tok_z.start()

    @pl.when(works)
    def _():
        for hop in range(1, chips):
            tok_copy(0, hop).start()
        hs_copy.start()
        for piece in range(pieces):
            gu_sib(piece, fs, True).start()
        dn_sib(fs, True).start()

    for way in (0, 1):
        own_copies(sc_side, way)

    @pl.when(fs == 0)
    def _():
        own_copies(dn_side, 0)

    @pl.when(fs == last)
    def _():
        own_copies(dn_side, 1)

    @pl.when(works)
    def _():
        tok_all[block(me), :] = tok_ref[...]
        tok_z.wait_recv()
        for hop in range(1, chips):
            tok_copy(1, hop).start()

    def arrive(make, source, way, to_sibling):
        make(source, way, False).wait_recv()

        @pl.when(goes(way))
        def _():
            make(source, way, False).start()

        if to_sibling is not None:

            @pl.when(works)
            def _():
                to_sibling(source, False).start()

    tile = 2 * rows
    tiles = chips

    def left_ok(step):
        return inside & (fs - step >= 0)

    def right_ok(step):
        return inside & (fs + step <= last)

    def gather_step(step, piece):
        from_left, from_right = fs - step, fs + step
        move, share = gu_part(piece)

        @pl.when(left_ok(step))
        def _():
            arrive(move, from_left, 0, share)

            if piece == pieces - 1:

                @pl.when(from_left == 0)
                def _():
                    own_copies(dn_side, 0)

        @pl.when(right_ok(step))
        def _():
            arrive(move, from_right, 1, share)

            if piece == pieces - 1:

                @pl.when(from_right == last)
                def _():
                    own_copies(dn_side, 1)

    def accumulate(piece, source, weights, fresh):
        gu_sib(piece, source, False).wait_recv()
        unit = source * pieces + piece

        def body(j, carry):
            r = pl.ds(pl.multiple_of(j * tile, tile), tile)
            k = pl.ds(pl.multiple_of(unit * depth, depth), depth)
            for c, block_of in ((0, weights), (1, gu_all.at[1, unit])):
                got = jnp.dot(tok_all[r, k], block_of[...], preferred_element_type=jnp.float32)
                acc[c, r, :] = got if fresh else acc[c, r, :] + got
            return carry

        lax.fori_loop(0, tiles, body, 0)

    for piece in range(pieces):
        gather_step(1, piece)

    @pl.when(works)
    def _():
        for hop in range(1, chips):
            for plane in (0, 1):
                tok_arrival(plane, (me + hop) % chips).wait_recv()
        for piece in range(pieces):
            accumulate(piece, fs, gu_ref.at[piece], piece == 0)

    def gu_step(step, carry):
        for piece in range(pieces):

            @pl.when(step > 1)
            def _():
                gather_step(step, piece)

            for source, ok in ((fs - step, left_ok(step)), (fs + step, right_ok(step))):

                @pl.when(works & ok)
                def _():
                    accumulate(piece, source, gu_all.at[0, source * pieces + piece], False)

        return carry

    lax.fori_loop(1, n_fs, gu_step, 0)

    @pl.when(works)
    def _():
        hs_copy.wait_recv()

        def activate(j, carry):
            r = block(j)
            for c, scale in ((0, hs_ref), (1, hs_all)):
                both = acc[c, r, :] * scale[0:1, :]
                gate, up = both[:, :half], both[:, half:]
                hidden[c, r, :] = (gate / (1.0 + jnp.exp(-gate)) * up).astype(jnp.bfloat16)
            return carry

        lax.fori_loop(0, 2 * chips, activate, 0)

    def part_copy(source, plane, to):
        return remote(
            parts.at[source, block(plane * chips + to), :],
            landed.at[source, plane, me],
            part_send.at[source, plane, to],
            part_recv.at[source, plane, me],
            chip(to),
        )

    def part_arrival(source, plane, index):
        return remote(
            parts.at[source, block(plane * chips + index), :],
            landed.at[source, plane, index],
            part_send.at[source, plane, index],
            part_recv.at[source, plane, index],
            chip(index),
        )

    def project(source, weights):
        dn_sib(source, False).wait_recv()

        def body(i, carry):
            j = tiles - 1 - i
            r = pl.ds(pl.multiple_of(j * tile, tile), tile)
            parts[source, r, :] = (
                jnp.dot(hidden[0, r, :], weights[...], preferred_element_type=jnp.float32)
                + jnp.dot(
                    hidden[1, r, :], dn_all[1, source], preferred_element_type=jnp.float32
                )
            ).astype(jnp.bfloat16)
            for k in (0, 1):
                index = j * 2 + k

                @pl.when(index % chips != me)
                def _():
                    part_copy(source, index // chips, index % chips).start()

            return carry

        lax.fori_loop(0, tiles, body, 0)

    def back_copy(source):
        return remote(
            back.at[source], back.at[source], back_send.at[source], back_recv.at[source], partner
        )

    def finish(source, scale):
        for plane in (1, 0):
            total = parts[source, block(plane * chips + me), :].astype(jnp.float32)
            for hop in range(1, chips):
                index = (me + hop) % chips
                part_arrival(source, plane, index).wait_recv()
                total = total + landed[source, plane, index].astype(jnp.float32)
            mixed = (total * scale).astype(jnp.bfloat16)
            if plane == 1:
                back[source] = mixed
                back_copy(source).start()
            else:
                out_ref[:, pl.ds(pl.multiple_of(source * cols, cols), cols)] = mixed

    @pl.when(works)
    def _():
        project(fs, dn_ref)

    def dn_step(step, carry):
        from_left, from_right = fs - step, fs + step

        @pl.when(left_ok(step))
        def _():
            arrive(sc_side, from_left, 0, None)
            arrive(dn_side, from_left, 0, dn_sib)

        @pl.when(right_ok(step))
        def _():
            arrive(sc_side, from_right, 1, None)
            arrive(dn_side, from_right, 1, dn_sib)

        @pl.when(works & left_ok(step))
        def _():
            project(from_left, dn_all.at[0, from_left])

        @pl.when(works & right_ok(step))
        def _():
            project(from_right, dn_all.at[0, from_right])

        return carry

    lax.fori_loop(1, n_fs, dn_step, 0)

    @pl.when(works)
    def _():
        finish(fs, ds_ref[0:1, :])

    def end_step(step, carry):
        for source, ok in ((fs - step, left_ok(step)), (fs + step, right_ok(step))):

            @pl.when(works & ok)
            def _():
                finish(source, sc_all[source, 0:1, :])

        return carry

    lax.fori_loop(1, n_fs, end_step, 0)

    @pl.when(jnp.logical_not(works))
    def _():
        tok_z.wait_send()

        def take(source, carry):
            back_copy(source).wait_recv()
            out_ref[:, pl.ds(pl.multiple_of(source * cols, cols), cols)] = back[source]
            return carry

        lax.fori_loop(0, n_fs, take, 0)

    def sent_step(source, carry):
        for make in [gu_part(piece)[0] for piece in range(pieces)] + [dn_side, sc_side]:

            @pl.when((source <= fs) & goes(0))
            def _():
                make(source, 0, False).wait_send()

            @pl.when((source >= fs) & goes(1))
            def _():
                make(source, 1, False).wait_send()

        @pl.when(works)
        def _():
            for piece in range(pieces):
                gu_sib(piece, source, False).wait_send()
            dn_sib(source, False).wait_send()
            back_copy(source).wait_send()
            for hop in range(1, chips):
                for plane in (0, 1):
                    part_copy(source, plane, (me + hop) % chips).wait_send()

        return carry

    lax.fori_loop(0, n_fs, sent_step, 0)

    @pl.when(works)
    def _():
        hs_copy.wait_send()
        for hop in range(1, chips):
            for plane in (0, 1):
                tok_copy(plane, hop).wait_send()


def shards(
    sizes,
    tokens,
    norm_gain,
    gate_weight,
    gate_scale,
    up_weight,
    up_scale,
    down_weight,
    down_scale,
):
    n_rep, n_fs, n_tp = sizes
    chips = n_rep * n_tp // 2
    width = gate_weight.shape[1] // n_rep
    begin = lax.axis_index("rep") * width

    def part(array, axis):
        return lax.dynamic_slice_in_dim(array, begin, width, axis)

    flat = tokens.astype(jnp.float32)
    mean_square = jnp.mean(flat * flat, axis=-1, keepdims=True)
    inverse = lax.rsqrt(mean_square + 1e-06)
    normed = (flat * inverse * norm_gain).astype(jnp.bfloat16)
    gu = jnp.concatenate(
        [part(gate_weight, 1).astype(jnp.bfloat16), part(up_weight, 1).astype(jnp.bfloat16)], axis=1
    )
    dn = part(down_weight, 0).astype(jnp.bfloat16)
    scale = jnp.broadcast_to(down_scale[None, :], (8, down_scale.shape[0]))
    hidden_scale = jnp.concatenate([part(gate_scale, 0), part(up_scale, 0)])
    hidden_scale = jnp.broadcast_to(hidden_scale[None, :], (8, 2 * width))
    rows, features = tokens.shape
    pieces = 2 if gu.shape[0] % 256 == 0 else 1
    depth = gu.shape[0] // pieces
    gu = gu.reshape(pieces, depth, 2 * width)
    cols = dn.shape[1]
    dma = pltpu.SemaphoreType.DMA
    vmem = pl.BlockSpec(memory_space=pltpu.VMEM)
    return pl.pallas_call(
        functools.partial(layer, n_rep, n_fs, n_tp),
        out_shape=jax.ShapeDtypeStruct((rows, features), jnp.bfloat16),
        in_specs=[vmem] * 5,
        out_specs=vmem,
        scratch_shapes=[
            pltpu.VMEM((2 * chips * rows, features), jnp.bfloat16),
            pltpu.VMEM((2, n_fs * pieces, depth, 2 * width), jnp.bfloat16),
            pltpu.VMEM((2, n_fs, width, cols), jnp.bfloat16),
            pltpu.VMEM((n_fs, 8, cols), jnp.float32),
            pltpu.VMEM((8, 2 * width), jnp.float32),
            pltpu.VMEM((2, 2 * chips * rows, 2 * width), jnp.float32),
            pltpu.VMEM((2, 2 * chips * rows, width), jnp.bfloat16),
            pltpu.VMEM((n_fs, 2 * chips * rows, cols), jnp.bfloat16),
            pltpu.VMEM((n_fs, 2, chips, rows, cols), jnp.bfloat16),
            pltpu.VMEM((n_fs, rows, cols), jnp.bfloat16),
            dma((2, chips)),
            dma((2, chips)),
            dma((2, n_fs * pieces)),
            dma((n_fs * pieces,)),
            dma((2, n_fs)),
            dma((n_fs,)),
            dma((2, n_fs)),
            dma((n_fs,)),
            dma((n_fs * pieces,)),
            dma((n_fs * pieces,)),
            dma((n_fs,)),
            dma((n_fs,)),
            dma((2,)),
            dma((n_fs, 2, chips)),
            dma((n_fs, 2, chips)),
            dma((n_fs,)),
            dma((n_fs,)),
            dma,
        ],
        compiler_params=pltpu.CompilerParams(
            collective_id=0, has_side_effects=True, vmem_limit_bytes=60 * 1024 * 1024
        ),
    )(normed, gu, dn, hidden_scale, scale)


def solution(mesh):
    in_specs = (
        P(("rep", "fs", "tp"), None),
        P(),
        P("fs", "tp"),
        P("tp"),
        P("fs", "tp"),
        P("tp"),
        P("tp", "fs"),
        P("fs"),
    )
    out_specs = P(("rep", "fs", "tp"), None)
    sizes = tuple(mesh.shape[axis] for axis in ("rep", "fs", "tp"))
    return jax.shard_map(
        functools.partial(shards, sizes),
        mesh=mesh,
        in_specs=in_specs,
        out_specs=out_specs,
        check_vma=False,
    )
```

```python
import functools

import jax
import jax.numpy as jnp
from jax import lax
from jax.experimental import pallas as pl
from jax.experimental.pallas import tpu as pltpu
from jax.sharding import PartitionSpec as P

MESH = pl.DeviceIdType.MESH


def layer(
    n_rep,
    n_fs,
    n_tp,
    tok_ref,
    gu_ref,
    dn_ref,
    hs_ref,
    ds_ref,
    out_ref,
    tok_all,
    gu_all,
    dn_all,
    sc_all,
    hs_all,
    acc,
    hidden,
    parts,
    landed,
    back,
    tok_send,
    tok_recv,
    gu_send,
    gu_recv,
    dn_send,
    dn_recv,
    sc_send,
    sc_recv,
    gu_sib_send,
    gu_sib_recv,
    dn_sib_send,
    dn_sib_recv,
    hs_sem,
    part_send,
    part_recv,
    back_send,
    back_recv,
    tok_z_send,
):
    rep, fs, tp = lax.axis_index("rep"), lax.axis_index("fs"), lax.axis_index("tp")
    n_row = n_tp // 2
    core = tp % 2
    chips = n_rep * n_row
    me = rep * n_row + tp // 2
    rows = tok_ref.shape[0]
    pieces = gu_ref.shape[0]
    depth = gu_ref.shape[1]
    half = gu_ref.shape[2] // 2
    cols = dn_ref.shape[1]
    low, high, last = 1, n_fs - 2, n_fs - 1
    pair = fs // 2
    parity = fs % 2
    upper = jnp.where(pair < n_fs // 4, 0, 1)
    works = parity + upper == 1
    inside = (fs >= low) & (fs <= high)
    partner = (rep, fs + 1 - 2 * parity, tp)
    sibling = (rep, fs, tp + 1 - 2 * core)

    def chip(index):
        return (index // n_row, fs, (index % n_row) * 2 + core)

    barrier = pltpu.get_barrier_semaphore()
    for hop in (1, n_fs - 1):
        pl.semaphore_signal(
            barrier, inc=1, device_id=(rep, (fs + hop) % n_fs, tp), device_id_type=MESH
        )
    pl.semaphore_signal(barrier, inc=1, device_id=sibling, device_id_type=MESH)
    for hop in range(1, chips):
        pl.semaphore_signal(
            barrier, inc=1, device_id=chip((me + hop) % chips), device_id_type=MESH
        )
    pl.semaphore_wait(barrier, chips + 2)

    def remote(src, dst, send, recv, device):
        return pltpu.make_async_remote_copy(
            src_ref=src,
            dst_ref=dst,
            send_sem=send,
            recv_sem=recv,
            device_id=device,
            device_id_type=MESH,
        )

    def block(index):
        return pl.ds(pl.multiple_of(index * rows, rows), rows)

    def side(own, store, send, recv, source, way, first):
        return remote(
            own if first else store.at[source],
            store.at[source],
            send.at[way, source],
            recv.at[source],
            (rep, (fs + (1, n_fs - 1)[way]) % n_fs, tp),
        )

    def gu_side(piece, source, way, first):
        unit = source * pieces + piece
        return remote(
            gu_ref.at[piece] if first else gu_all.at[0, unit],
            gu_all.at[0, unit],
            gu_send.at[way, unit],
            gu_recv.at[unit],
            (rep, (fs + (1, n_fs - 1)[way]) % n_fs, tp),
        )

    dn_side = functools.partial(side, dn_ref, dn_all.at[0], dn_send, dn_recv)
    sc_side = functools.partial(side, ds_ref, sc_all, sc_send, sc_recv)

    def sib(own, store, send, recv, source, first):
        return remote(
            own if first else store.at[0, source],
            store.at[1, source],
            send.at[source],
            recv.at[source],
            sibling,
        )

    def gu_sib(piece, source, first):
        unit = source * pieces + piece
        return sib(gu_ref.at[piece], gu_all, gu_sib_send, gu_sib_recv, unit, first)

    def gu_part(piece):
        return functools.partial(gu_side, piece), functools.partial(gu_sib, piece)

    dn_sib = functools.partial(sib, dn_ref, dn_all, dn_sib_send, dn_sib_recv)
    hs_copy = remote(hs_ref, hs_all, hs_sem.at[0], hs_sem.at[1], sibling)

    def goes(way):
        return fs < high if way == 0 else fs > low

    def own_copies(make, way):
        @pl.when(goes(way))
        def _():
            make(fs, way, True).start()

    def tok_copy(plane, hop):
        to = (me + hop) % chips
        home = tok_all.at[block(plane * chips + me), :]
        return remote(
            tok_ref if plane == 0 else home,
            home,
            tok_send.at[plane, to],
            tok_recv.at[plane, me],
            chip(to),
        )

    def tok_arrival(plane, index):
        home = tok_all.at[block(plane * chips + index), :]
        return remote(
            home, home, tok_send.at[plane, index], tok_recv.at[plane, index], chip(index)
        )

    tok_z = remote(
        tok_ref, tok_all.at[block(chips + me), :], tok_z_send, tok_recv.at[1, me], partner
    )

    for piece in range(pieces):
        for way in (0, 1):
            own_copies(gu_part(piece)[0], way)
        if piece == 0:

            @pl.when(jnp.logical_not(works))
            def _():
                tok_z.start()

    @pl.when(works)
    def _():
        for hop in range(1, chips):
            tok_copy(0, hop).start()
        hs_copy.start()
        for piece in range(pieces):
            gu_sib(piece, fs, True).start()
        dn_sib(fs, True).start()

    for way in (0, 1):
        own_copies(sc_side, way)

    @pl.when(fs == 0)
    def _():
        own_copies(dn_side, 0)

    @pl.when(fs == last)
    def _():
        own_copies(dn_side, 1)

    @pl.when(works)
    def _():
        tok_all[block(me), :] = tok_ref[...]
        tok_z.wait_recv()
        for hop in range(1, chips):
            tok_copy(1, hop).start()

    def arrive(make, source, way, to_sibling):
        make(source, way, False).wait_recv()

        @pl.when(goes(way))
        def _():
            make(source, way, False).start()

        if to_sibling is not None:

            @pl.when(works)
            def _():
                to_sibling(source, False).start()

    tile = 2 * rows
    tiles = chips

    def left_ok(step):
        return inside & (fs - step >= 0)

    def right_ok(step):
        return inside & (fs + step <= last)

    def gather_step(step, piece):
        from_left, from_right = fs - step, fs + step
        move, share = gu_part(piece)

        @pl.when(left_ok(step))
        def _():
            arrive(move, from_left, 0, share)

            if piece == pieces - 1:

                @pl.when(from_left == 0)
                def _():
                    own_copies(dn_side, 0)

        @pl.when(right_ok(step))
        def _():
            arrive(move, from_right, 1, share)

            if piece == pieces - 1:

                @pl.when(from_right == last)
                def _():
                    own_copies(dn_side, 1)

    def accumulate(piece, source, weights, fresh):
        gu_sib(piece, source, False).wait_recv()
        unit = source * pieces + piece

        def body(j, carry):
            r = pl.ds(pl.multiple_of(j * tile, tile), tile)
            k = pl.ds(pl.multiple_of(unit * depth, depth), depth)
            for c, block_of in ((0, weights), (1, gu_all.at[1, unit])):
                got = jnp.dot(tok_all[r, k], block_of[...], preferred_element_type=jnp.float32)
                acc[c, r, :] = got if fresh else acc[c, r, :] + got
            return carry

        lax.fori_loop(0, tiles, body, 0)

    for piece in range(pieces):
        gather_step(1, piece)

    @pl.when(works)
    def _():
        for hop in range(1, chips):
            for plane in (0, 1):
                tok_arrival(plane, (me + hop) % chips).wait_recv()
        for piece in range(pieces):
            accumulate(piece, fs, gu_ref.at[piece], piece == 0)

    def gu_step(step, carry):
        for piece in range(pieces):

            @pl.when(step > 1)
            def _():
                gather_step(step, piece)

            for source, ok in ((fs - step, left_ok(step)), (fs + step, right_ok(step))):

                @pl.when(works & ok)
                def _():
                    accumulate(piece, source, gu_all.at[0, source * pieces + piece], False)

        return carry

    lax.fori_loop(1, n_fs, gu_step, 0)

    def activate(index):
        r = block(index)
        for c, scale in ((0, hs_ref), (1, hs_all)):
            both = acc[c, r, :] * scale[0:1, :]
            gate, up = both[:, :half], both[:, half:]
            hidden[c, r, :] = (gate / (1.0 + jnp.exp(-gate)) * up).astype(jnp.bfloat16)

    def part_copy(source, plane, to):
        return remote(
            parts.at[source, block(plane * chips + to), :],
            landed.at[source, plane, me],
            part_send.at[source, plane, to],
            part_recv.at[source, plane, me],
            chip(to),
        )

    def part_arrival(source, plane, index):
        return remote(
            parts.at[source, block(plane * chips + index), :],
            landed.at[source, plane, index],
            part_send.at[source, plane, index],
            part_recv.at[source, plane, index],
            chip(index),
        )

    def project(source, weights, fresh):
        dn_sib(source, False).wait_recv()

        def body(i, carry):
            j = tiles - 1 - i
            r = pl.ds(pl.multiple_of(j * tile, tile), tile)
            if fresh:
                for k in (0, 1):
                    activate(j * 2 + k)
            parts[source, r, :] = (
                jnp.dot(hidden[0, r, :], weights[...], preferred_element_type=jnp.float32)
                + jnp.dot(
                    hidden[1, r, :], dn_all[1, source], preferred_element_type=jnp.float32
                )
            ).astype(jnp.bfloat16)
            for k in (0, 1):
                index = j * 2 + k

                @pl.when(index % chips != me)
                def _():
                    part_copy(source, index // chips, index % chips).start()

            return carry

        lax.fori_loop(0, tiles, body, 0)

    def back_copy(source):
        return remote(
            back.at[source], back.at[source], back_send.at[source], back_recv.at[source], partner
        )

    def finish(source, scale):
        for plane in (1, 0):
            total = parts[source, block(plane * chips + me), :].astype(jnp.float32)
            for hop in range(1, chips):
                index = (me + hop) % chips
                part_arrival(source, plane, index).wait_recv()
                total = total + landed[source, plane, index].astype(jnp.float32)
            mixed = (total * scale).astype(jnp.bfloat16)
            if plane == 1:
                back[source] = mixed
                back_copy(source).start()
            else:
                out_ref[:, pl.ds(pl.multiple_of(source * cols, cols), cols)] = mixed

    @pl.when(works)
    def _():
        hs_copy.wait_recv()
        project(fs, dn_ref, True)

    def dn_step(step, carry):
        from_left, from_right = fs - step, fs + step

        @pl.when(left_ok(step))
        def _():
            arrive(sc_side, from_left, 0, None)
            arrive(dn_side, from_left, 0, dn_sib)

        @pl.when(right_ok(step))
        def _():
            arrive(sc_side, from_right, 1, None)
            arrive(dn_side, from_right, 1, dn_sib)

        @pl.when(works & left_ok(step))
        def _():
            project(from_left, dn_all.at[0, from_left], False)

        @pl.when(works & right_ok(step))
        def _():
            project(from_right, dn_all.at[0, from_right], False)

        return carry

    lax.fori_loop(1, n_fs, dn_step, 0)

    @pl.when(works)
    def _():
        finish(fs, ds_ref[0:1, :])

    def end_step(step, carry):
        for source, ok in ((fs - step, left_ok(step)), (fs + step, right_ok(step))):

            @pl.when(works & ok)
            def _():
                finish(source, sc_all[source, 0:1, :])

        return carry

    lax.fori_loop(1, n_fs, end_step, 0)

    @pl.when(jnp.logical_not(works))
    def _():
        tok_z.wait_send()

        def take(source, carry):
            back_copy(source).wait_recv()
            out_ref[:, pl.ds(pl.multiple_of(source * cols, cols), cols)] = back[source]
            return carry

        lax.fori_loop(0, n_fs, take, 0)

    def sent_step(source, carry):
        for make in [gu_part(piece)[0] for piece in range(pieces)] + [dn_side, sc_side]:

            @pl.when((source <= fs) & goes(0))
            def _():
                make(source, 0, False).wait_send()

            @pl.when((source >= fs) & goes(1))
            def _():
                make(source, 1, False).wait_send()

        @pl.when(works)
        def _():
            for piece in range(pieces):
                gu_sib(piece, source, False).wait_send()
            dn_sib(source, False).wait_send()
            back_copy(source).wait_send()
            for hop in range(1, chips):
                for plane in (0, 1):
                    part_copy(source, plane, (me + hop) % chips).wait_send()

        return carry

    lax.fori_loop(0, n_fs, sent_step, 0)

    @pl.when(works)
    def _():
        hs_copy.wait_send()
        for hop in range(1, chips):
            for plane in (0, 1):
                tok_copy(plane, hop).wait_send()


def shards(
    sizes,
    tokens,
    norm_gain,
    gate_weight,
    gate_scale,
    up_weight,
    up_scale,
    down_weight,
    down_scale,
):
    n_rep, n_fs, n_tp = sizes
    chips = n_rep * n_tp // 2
    width = gate_weight.shape[1] // n_rep
    begin = lax.axis_index("rep") * width

    def part(array, axis):
        return lax.dynamic_slice_in_dim(array, begin, width, axis)

    flat = tokens.astype(jnp.float32)
    mean_square = jnp.mean(flat * flat, axis=-1, keepdims=True)
    inverse = lax.rsqrt(mean_square + 1e-06)
    normed = (flat * inverse * norm_gain).astype(jnp.bfloat16)
    gu = jnp.concatenate(
        [part(gate_weight, 1).astype(jnp.bfloat16), part(up_weight, 1).astype(jnp.bfloat16)], axis=1
    )
    dn = part(down_weight, 0).astype(jnp.bfloat16)
    scale = jnp.broadcast_to(down_scale[None, :], (8, down_scale.shape[0]))
    hidden_scale = jnp.concatenate([part(gate_scale, 0), part(up_scale, 0)])
    hidden_scale = jnp.broadcast_to(hidden_scale[None, :], (8, 2 * width))
    rows, features = tokens.shape
    pieces = 2 if gu.shape[0] % 256 == 0 else 1
    depth = gu.shape[0] // pieces
    gu = gu.reshape(pieces, depth, 2 * width)
    cols = dn.shape[1]
    dma = pltpu.SemaphoreType.DMA
    vmem = pl.BlockSpec(memory_space=pltpu.VMEM)
    return pl.pallas_call(
        functools.partial(layer, n_rep, n_fs, n_tp),
        out_shape=jax.ShapeDtypeStruct((rows, features), jnp.bfloat16),
        in_specs=[vmem] * 5,
        out_specs=vmem,
        scratch_shapes=[
            pltpu.VMEM((2 * chips * rows, features), jnp.bfloat16),
            pltpu.VMEM((2, n_fs * pieces, depth, 2 * width), jnp.bfloat16),
            pltpu.VMEM((2, n_fs, width, cols), jnp.bfloat16),
            pltpu.VMEM((n_fs, 8, cols), jnp.float32),
            pltpu.VMEM((8, 2 * width), jnp.float32),
            pltpu.VMEM((2, 2 * chips * rows, 2 * width), jnp.float32),
            pltpu.VMEM((2, 2 * chips * rows, width), jnp.bfloat16),
            pltpu.VMEM((n_fs, 2 * chips * rows, cols), jnp.bfloat16),
            pltpu.VMEM((n_fs, 2, chips, rows, cols), jnp.bfloat16),
            pltpu.VMEM((n_fs, rows, cols), jnp.bfloat16),
            dma((2, chips)),
            dma((2, chips)),
            dma((2, n_fs * pieces)),
            dma((n_fs * pieces,)),
            dma((2, n_fs)),
            dma((n_fs,)),
            dma((2, n_fs)),
            dma((n_fs,)),
            dma((n_fs * pieces,)),
            dma((n_fs * pieces,)),
            dma((n_fs,)),
            dma((n_fs,)),
            dma((2,)),
            dma((n_fs, 2, chips)),
            dma((n_fs, 2, chips)),
            dma((n_fs,)),
            dma((n_fs,)),
            dma,
        ],
        compiler_params=pltpu.CompilerParams(
            collective_id=0, has_side_effects=True, vmem_limit_bytes=60 * 1024 * 1024
        ),
    )(normed, gu, dn, hidden_scale, scale)


def solution(mesh):
    in_specs = (
        P(("rep", "fs", "tp"), None),
        P(),
        P("fs", "tp"),
        P("tp"),
        P("fs", "tp"),
        P("tp"),
        P("tp", "fs"),
        P("fs"),
    )
    out_specs = P(("rep", "fs", "tp"), None)
    sizes = tuple(mesh.shape[axis] for axis in ("rep", "fs", "tp"))
    return jax.shard_map(
        functools.partial(shards, sizes),
        mesh=mesh,
        in_specs=in_specs,
        out_specs=out_specs,
        check_vma=False,
    )
```
